512 devices in a mesh: gr: 2 (over z_hi), fs: 32 (over z_lo, y), tp: 8 (over x, core).
Axes of the slice: x: 4, y: 4, z: 16 (z_hi: 2, z_lo: 8; z = z_hi * 8 + z_lo), core: 2. Of those that a mesh axis runs over, the one named last changes fastest.
Arguments:
- tokens: bfloat16 [8192, 2048], P(('gr', 'fs')), may hold values from -60 to 60
- route_ids: int32 [8192, 2], P(('gr', 'fs')), may hold values from 0 to 7, all different within a row; in each aligned block of 128 rows (0 to 127, 128 to 255, ...) at most 32 rows name the same one
- route_logits: float32 [8192, 2], P(('gr', 'fs')), may hold values from -8 to 8
- norm_gain: float32 [2048], P(('gr', 'fs')), may hold values from 0.1 to 1.9
- gate_master: float32 [8, 2048, 7168], P(None, ('gr', 'fs'), 'tp'), may hold values from -0.125 to 0.125
- up_master: float32 [8, 2048, 7168], P(None, ('gr', 'fs'), 'tp'), may hold values from -0.125 to 0.125
- down_master: float32 [8, 7168, 2048], P(None, 'fs', ('gr', 'tp')), may hold values from -0.0625 to 0.0625
Outputs:
- gate_weight: bfloat16 [8, 2048, 7168], P('tp', None, 'fs')
- up_weight: bfloat16 [8, 2048, 7168], P('tp', None, 'fs')
- down_weight: bfloat16 [8, 7168, 2048], P('tp', 'fs')
- mixed: bfloat16 [8192, 2048], P(('gr', 'fs'))
The draws below stay inside these ranges and needn't reach their ends.
Inputs may be any that keep to these rules, and one draw needn't show every extreme that they name: `route_ids`: in the rows of one device, that is in each aligned block of 128 rows, each of the 8 experts is named by exactly 32 rows; a row names two different experts.
All inputs are finite; a program needn't handle non-finite values.
Results may differ from the reference program's by a relative error of at most 0.025.
Values may be sent and summed in bfloat16 or wider, within the bound.
No kernel may reach another device: no remote copies, remote signals or barrier semaphores. Data moves between devices by JAX's collectives and lax.ppermute only.
A program may use at most 64 MiB of HBM per device.

```python
import math
import jax
import jax.numpy as jnp
import numpy as np
from jax import lax

D = 2048
FF = 7168
EXPERTS = 8
TOK_DEV = 128
CAP = 32
TOKENS = 8192
N_FS = 32
N_TP = 8


def draw_tokens(key, part):
    first_key = jax.random.fold_in(key, 11)
    second_key = jax.random.fold_in(key, 12)
    values = jnp.clip(jax.random.normal(first_key, (TOKENS, D), jnp.float32), -4.0, 4.0)
    scales = jnp.exp(jax.random.uniform(second_key, (TOKENS, 1), jnp.float32, 0.0, math.log(10.0)))
    return (values * scales).astype(jnp.bfloat16)


def level_of(own_key, shape, pieces, smallest, largest):
    loudness, own = 1.0, jax.random.fold_in(own_key, 6)
    for position, parts in pieces:
        heights = jnp.exp(jax.random.uniform(jax.random.fold_in(own, position), (parts,), jnp.float32, smallest / len(pieces), largest / len(pieces)))
        loudness = loudness * jnp.repeat(heights, shape[position] // parts).reshape([-1 if axis == position else 1 for axis in range(len(shape))])
    return loudness


def shared_out(rng, own, number, rows, count, top, reach, lean):
    order = jax.random.permutation(rng, count)
    crowded, usual = portions_of(count, rows * top, reach, lean, True), portions_of(count, rows * top, reach, lean, False)
    places = jnp.arange(count)

    def named(tallies, rotation):
        used = int((tallies > 0).sum())
        fixed = max(1, used // 4)
        passed = fixed + (places - fixed + rotation * (used - fixed)) % max(1, count - fixed)
        return jnp.zeros((count,), jnp.int32).at[order[jnp.where(places < fixed, places, passed)]].set(jnp.asarray(tallies, jnp.int32))

    tallies = jnp.where(number % 4 == 0, named(crowded, number // 4), named(usual, number - number // 4 - 1))
    mixed = jax.random.permutation(jax.random.fold_in(own, 3), count)
    giver, sink = mixed[0:count // 2 * 2:2], mixed[1:count // 2 * 2:2]
    margin = jnp.minimum(tallies[giver] - 1, reach - tallies[sink]) // 2
    margin = jnp.where((giver == order[0]) | (sink == order[0]) | (tallies[sink] == 0), 0, jnp.maximum(margin, 0))
    passed = jax.random.randint(jax.random.fold_in(own, 4), (count // 2,), 0, 1 << 20) % (margin + 1)
    tallies = tallies.at[giver].add(-passed).at[sink].add(passed)
    labels = jnp.searchsorted(jnp.cumsum(tallies), jnp.arange(rows * top), side="right").astype(jnp.int32)
    table = labels.reshape(top, rows).T
    table = table[jax.random.permutation(jax.random.fold_in(own, 1), rows)]
    rotation = jax.random.randint(jax.random.fold_in(own, 2), (rows, 1), 0, top)
    return jnp.take_along_axis(table, (jnp.arange(top)[None, :] + rotation) % top, axis=1)


def portions_of(number_of, total, reach, slope, full):
    portions = [(1 << 20) // math.isqrt(rank ** slope) + 1 for rank in range(1, number_of + 1)]
    largest = reach if full else min(reach, max(-(-total // number_of), total * portions[0] // sum(portions)))
    least = 1 if total - largest >= number_of - 1 else 0
    holding, rest = [largest] + [least] * (number_of - 1), total - largest - least * (number_of - 1)
    while rest > 0:
        movable = [i for i in range(1, number_of) if holding[i] < largest] or [i for i in range(1, number_of) if holding[i] < reach]
        whole, budget = sum([portions[i] for i in movable]), rest
        for i in movable:
            extra = min(reach - holding[i], max(1, budget * portions[i] // whole), rest)
            holding[i] = holding[i] + extra
            rest = rest - extra
    return np.array(holding)


def scatter_about(stream_key, dims, scale, limit, cuts=(), kind=jnp.bfloat16):
    loudness = level_of(stream_key, dims, cuts, -0.22, 0.18) if cuts else 1.0
    array = jax.random.normal(stream_key, dims, jnp.float32) * scale * loudness
    return jnp.minimum(jnp.maximum(array, -limit), limit).astype(kind)


def setup_inputs(seed: int = 0) -> dict:
    keys = jax.random.split(jax.random.key(seed), 8)
    tokens = draw_tokens(jax.random.fold_in(keys[7], 71), 0)
    route_ids_keys = jax.random.split(jax.random.fold_in(keys[1], 1), TOKENS // TOK_DEV)
    route_ids_turns = jax.random.permutation(jax.random.fold_in(keys[1], 3), TOKENS // TOK_DEV)
    route_ids = jax.vmap(lambda own, number: shared_out(jax.random.fold_in(keys[1], 2), own, number, TOK_DEV, EXPERTS, 2, CAP, 1))(route_ids_keys, route_ids_turns).reshape((TOKENS, 2))
    route_logits = scatter_about(keys[2], (TOKENS, 2), 1.5, 8.0, ((0, 64),), jnp.float32)
    norm_gain = jnp.clip(1.0 + 0.18 * jax.random.normal(keys[3], (D,), jnp.float32), 0.1, 1.9)
    gate_master = scatter_about(keys[4], (EXPERTS, D, FF), D ** -0.5, 0.125, ((1, 64), (2, 8)), jnp.float32)
    up_master = scatter_about(keys[5], (EXPERTS, D, FF), D ** -0.5, 0.125, ((1, 64), (2, 8)), jnp.float32)
    down_master = scatter_about(keys[6], (EXPERTS, FF, D), FF ** -0.5, 0.0625, ((1, 32), (2, 16)), jnp.float32)
    return {"tokens": tokens, "route_ids": route_ids, "route_logits": route_logits, "norm_gain": norm_gain, "gate_master": gate_master, "up_master": up_master, "down_master": down_master}


epsilon = 1e-06

def reference(tokens, route_ids, route_logits, norm_gain, gate_master, up_master, down_master):
    gate_weight = (gate_master * norm_gain[None, :, None]).astype(jnp.bfloat16)
    up_weight = (up_master * norm_gain[None, :, None]).astype(jnp.bfloat16)
    down_weight = down_master.astype(jnp.bfloat16)
    as_float = tokens.astype(jnp.float32)
    normed = (as_float * lax.rsqrt(lax.optimization_barrier(jnp.mean(as_float * as_float, axis=-1, keepdims=True)) + epsilon)).astype(jnp.bfloat16)
    differ = route_logits[:, 0] - route_logits[:, 1]
    route_weight = jnp.stack([jax.nn.sigmoid(differ), jax.nn.sigmoid(-differ)], axis=1)
    routed = TOKENS // 4
    positions = jnp.arange(TOKENS, dtype=jnp.int32)
    slice_width = FF // N_FS
    per_block = EXPERTS // N_TP

    def expert_part(expert):
        route_hits = route_ids == expert
        chosen = jnp.any(route_hits, axis=1)
        sort_key = jnp.where(chosen, positions, positions + TOKENS)
        order = jnp.argsort(sort_key)[:routed].astype(jnp.int32)
        weight_rows = lax.optimization_barrier(jnp.sum(jnp.where(route_hits, route_weight, 0.0), axis=1))[order]
        picked = normed[order]
        gate_act = jnp.dot(picked, gate_weight[expert], preferred_element_type=jnp.float32)
        up_act = jnp.dot(picked, up_weight[expert], preferred_element_type=jnp.float32)
        hidden = (jax.nn.silu(gate_act) * up_act).astype(jnp.bfloat16)
        down_expert = down_weight[expert]

        def add_slice(summed, slice_idx):
            begin = (slice_idx * slice_width).astype(jnp.int32)
            hidden_slice = lax.dynamic_slice_in_dim(hidden, begin, slice_width, 1)
            down_slice = lax.dynamic_slice_in_dim(down_expert, begin, slice_width, 0)
            partial_value = jnp.dot(hidden_slice, down_slice, preferred_element_type=jnp.float32)
            rounded = lax.optimization_barrier(partial_value.astype(jnp.bfloat16)).astype(jnp.float32)
            return (summed + rounded, None)
        expert_out, _ = lax.scan(add_slice, jnp.zeros((routed, D), jnp.float32), jnp.arange(N_FS, dtype=jnp.int32))
        return jnp.zeros((TOKENS, D), jnp.float32).at[order].add(expert_out * weight_rows[:, None])
    summed_all = jnp.zeros((TOKENS, D), jnp.float32)
    for tp_block in range(N_TP):
        block_sum = jnp.zeros((TOKENS, D), jnp.float32)
        for member in range(per_block):
            block_sum = block_sum + expert_part(tp_block * per_block + member)
        summed_all = summed_all + lax.optimization_barrier(block_sum.astype(jnp.bfloat16)).astype(jnp.float32)
    mixed = summed_all.astype(jnp.bfloat16)
    return (gate_weight, up_weight, down_weight, mixed)
```

```python
import jax
import jax.numpy as jnp
from jax import lax
from jax.experimental import pallas as pl
from jax.experimental.pallas import tpu as pltpu
from jax.sharding import Mesh
from jax.sharding import PartitionSpec as P

CAP = 32
FS = ("fs_0", "fs_1")
GR_FS = ("gr", "fs_0", "fs_1")
ALL = ("gr", "fs_0", "fs_1", "tp")
EPS = 1e-06
LANES = 128


def lane_window(blocks, start):
    first, offset = divmod(start, LANES)
    if offset == 0:
        return blocks[first]
    head = pltpu.roll(blocks[first], LANES - offset, 1)
    if first + 1 == len(blocks):
        return head
    rest = pltpu.roll(blocks[first + 1], LANES - offset, 1)
    lane = lax.broadcasted_iota(jnp.int32, head.shape, 1)
    return jnp.where(lane < LANES - offset, head, rest)


def pack_kernel(gate_ref, up_ref, gain_ref, out_ref):
    gain = gain_ref[...]
    both = jnp.concatenate([gate_ref[0] * gain, up_ref[0] * gain], axis=0)
    blocks = [both[:, LANES * b : LANES * (b + 1)] for b in range(both.shape[1] // LANES)]
    lane = lax.broadcasted_iota(jnp.int32, (48, LANES), 1)
    for j in range(4):
        main = lane_window(blocks, 224 * j)
        tail = lane_window(blocks, 224 * j + LANES)
        last = tail[48:]
        spread = jnp.concatenate([pltpu.roll(last, 96 - 32 * q, 1) for q in range(3)], axis=0)
        out_ref[0, j, :64, :] = main.astype(jnp.bfloat16)
        out_ref[0, j, 64:, :] = jnp.where(lane < 96, tail[:48], spread).astype(jnp.bfloat16)


def pack(gate_master, up_master, gain):
    experts, rows, cols = gate_master.shape
    return pl.pallas_call(
        pack_kernel,
        grid=(experts,),
        in_specs=[
            pl.BlockSpec((1, rows, cols), lambda i: (i, 0, 0)),
            pl.BlockSpec((1, rows, cols), lambda i: (i, 0, 0)),
            pl.BlockSpec((rows, 1), lambda i: (0, 0)),
        ],
        out_specs=pl.BlockSpec((1, 4, 112, LANES), lambda i: (i, 0, 0, 0)),
        out_shape=jax.ShapeDtypeStruct((experts, 4, 112, LANES), jnp.bfloat16),
        cost_estimate=pl.CostEstimate(flops=4000000, bytes_accessed=2800000, transcendentals=0),
        compiler_params=pltpu.CompilerParams(vmem_limit_bytes=4 * 2**20),
        name="pack",
    )(gate_master, up_master, gain)


def unpack_kernel(tiles_ref, gate_ref, up_ref):
    lane = lax.broadcasted_iota(jnp.int32, (16, LANES), 1)
    for s in range(tiles_ref.shape[0]):
        rows = pl.ds(32 * s, 32)
        gate_ref[0, rows, :LANES] = tiles_ref[s, 0:32, :]
        up_ref[0, rows, :LANES] = tiles_ref[s, 32:64, :]
        gate_ref[0, rows, LANES:] = tiles_ref[s, 64:96, :96]
        up_ref[0, pl.ds(32 * s, 16), LANES:] = tiles_ref[s, 96:112, :96]
        parts = [
            pltpu.roll(
                tiles_ref[s, 64 + 16 * q : 80 + 16 * q, :].astype(jnp.float32), 32 * q + 32, 1
            )
            for q in range(3)
        ]
        last = jnp.where(lane < 32, parts[0], jnp.where(lane < 64, parts[1], parts[2]))
        up_ref[0, pl.ds(32 * s + 16, 16), LANES:] = last[:, :96].astype(jnp.bfloat16)


def unpack(tiles):
    count = tiles.shape[0]
    step = 16
    out = jax.ShapeDtypeStruct((1, 32 * count, 224), jnp.bfloat16)
    return pl.pallas_call(
        unpack_kernel,
        grid=(count // step,),
        in_specs=[pl.BlockSpec((step, 112, LANES), lambda i: (i, 0, 0))],
        out_specs=[pl.BlockSpec((1, 32 * step, 224), lambda i: (0, i, 0))] * 2,
        out_shape=[out, out],
        cost_estimate=pl.CostEstimate(flops=2000000, bytes_accessed=3800000, transcendentals=0),
        compiler_params=pltpu.CompilerParams(vmem_limit_bytes=6 * 2**20),
        name="unpack",
    )(tiles)


def permutation(sizes, move):
    groups, fs_0, fs_1, tp = sizes
    pairs = []
    for g in range(groups):
        for a in range(fs_0):
            for b in range(fs_1):
                for t in range(tp):
                    z, y = move(g * fs_0 + a, b, t)
                    z, y = z % (groups * fs_0), y % fs_1
                    pairs.append((((g * fs_0 + a) * fs_1 + b) * tp + t, (z * fs_1 + y) * tp + t))
    return pairs


def local(sizes, tokens, route_ids, route_logits, norm_gain, gate_master, up_master, down_master):
    f32, bf16 = jnp.float32, jnp.bfloat16
    fs_1, tp_size = sizes[2], sizes[3]

    def along_z(x, hops):
        pairs = permutation(sizes, lambda z, y, t: (z + (hops if t % 2 == 0 else -hops), y))
        return lax.ppermute(x, ALL, pairs)

    def along_y(x, hops):
        return lax.ppermute(x, ALL, permutation(sizes, lambda z, y, t: (z, y + hops)))

    as_float = tokens.astype(f32)
    normed = (
        as_float * lax.rsqrt(jnp.mean(as_float * as_float, axis=-1, keepdims=True) + EPS)
    ).astype(bf16)
    differ = route_logits[:, 0] - route_logits[:, 1]
    route_weight = jnp.stack([jax.nn.sigmoid(differ), jax.nn.sigmoid(-differ)], axis=1)
    expert_ids = jnp.arange(tp_size, dtype=jnp.int32)
    route_hits = route_ids[None, :, :] == expert_ids[:, None, None]
    chosen = jnp.any(route_hits, axis=2)
    slot_rank = jnp.cumsum(chosen.astype(jnp.int32), axis=1) - 1
    slot_ids = jnp.arange(CAP, dtype=jnp.int32)
    picker = chosen[:, None, :] & (slot_rank[:, None, :] == slot_ids[None, :, None])
    weight_rows = jnp.sum(jnp.where(route_hits, route_weight[None, :, :], 0.0), axis=2)
    mine = lax.axis_index("tp")
    my_picker = lax.dynamic_index_in_dim(picker, mine, 0, keepdims=False)
    my_weights = lax.dynamic_index_in_dim(weight_rows, mine, 0, keepdims=False)
    slot_weight = jnp.sum(jnp.where(my_picker, my_weights[None, :], 0.0), axis=1)
    packed = jnp.dot(my_picker.astype(bf16), normed, preferred_element_type=f32).astype(bf16)

    held = packed
    for hops in (4, 2, 1):
        held = jnp.concatenate([held, along_z(held, hops)], axis=0)
    pieces = [held] + [along_y(held, k) for k in range(1, fs_1)]

    down_half = down_master.astype(bf16)
    down_tiles = lax.all_to_all(
        jnp.concatenate([down_half, down_half], axis=0), ("gr", "tp"), 0, 0, tiled=True
    )
    down_weight = jnp.moveaxis(down_tiles, 0, 1).reshape(1, down_half.shape[1], -1)
    tiles = pack(gate_master, up_master, norm_gain[:, None])
    tiles = lax.all_to_all(tiles, "tp", 0, 0, tiled=True).reshape(-1, 112, LANES)
    tiles = lax.all_to_all(
        jnp.concatenate([tiles, tiles], axis=0), GR_FS, 0, 0, tiled=True
    )
    gate_weight, up_weight = unpack(tiles)

    partial = []
    for piece in pieces:
        gate_act = jnp.dot(piece, gate_weight[0], preferred_element_type=f32)
        up_act = jnp.dot(piece, up_weight[0], preferred_element_type=f32)
        hidden = (jax.nn.silu(gate_act) * up_act).astype(bf16)
        partial.append(jnp.dot(hidden, down_weight[0], preferred_element_type=f32).astype(bf16))
    total = partial[0].astype(f32)
    for k in range(1, fs_1):
        total = total + along_y(partial[k], -k).astype(f32)
    for hops in (1, 2, 4):
        half = total.shape[0] // 2
        total = total[:half] + along_z(total[half:].astype(bf16), -hops).astype(f32)
    block = (total * slot_weight[:, None]).astype(bf16)
    blocks = lax.all_to_all(
        jnp.broadcast_to(block[None], (tp_size, *block.shape)), "tp", 0, 0, tiled=True
    )
    mixed = lax.dot_general(
        picker.reshape(-1, picker.shape[2]).astype(bf16),
        blocks.reshape(-1, blocks.shape[2]),
        (((0,), (0,)), ((), ())),
        preferred_element_type=f32,
    ).astype(bf16)
    return (gate_weight, up_weight, down_weight, mixed)


def solution(mesh):
    sizes = (mesh.shape["gr"], 8, 4, mesh.shape["tp"])
    torus = Mesh(mesh.devices.reshape(sizes), ALL)
    in_specs = (
        P(GR_FS, None),
        P(GR_FS, None),
        P(GR_FS, None),
        P(GR_FS),
        P(None, GR_FS, "tp"),
        P(None, GR_FS, "tp"),
        P(None, FS, ("gr", "tp")),
    )
    out_specs = (P("tp", None, FS), P("tp", None, FS), P("tp", FS, None), P(GR_FS, None))

    def call(*arrays):
        return local(sizes, *arrays)

    return jax.shard_map(call, mesh=torus, in_specs=in_specs, out_specs=out_specs, check_vma=False)
```

```python
import jax
import jax.numpy as jnp
from jax import lax
from jax.experimental import pallas as pl
from jax.experimental.pallas import tpu as pltpu
from jax.sharding import Mesh
from jax.sharding import PartitionSpec as P


CAP = 32
FS = ("fs_0", "fs_1")
GR_FS = ("gr", "fs_0", "fs_1")
ALL = ("gr", "fs_0", "fs_1", "tp")
EPS = 1e-06
LANES = 128


def lane_window(blocks, start):
    first, offset = divmod(start, LANES)
    if offset == 0:
        return blocks[first]
    head = pltpu.roll(blocks[first], LANES - offset, 1)
    if first + 1 == len(blocks):
        return head
    rest = pltpu.roll(blocks[first + 1], LANES - offset, 1)
    lane = lax.broadcasted_iota(jnp.int32, head.shape, 1)
    return jnp.where(lane < LANES - offset, head, rest)


def pack_kernel(gate_ref, up_ref, gain_ref, out_ref):
    gain = gain_ref[...]
    both = jnp.concatenate([gate_ref[0] * gain, up_ref[0] * gain], axis=0)
    blocks = [both[:, LANES * b : LANES * (b + 1)] for b in range(both.shape[1] // LANES)]
    lane = lax.broadcasted_iota(jnp.int32, (48, LANES), 1)
    for j in range(4):
        main = lane_window(blocks, 224 * j)
        tail = lane_window(blocks, 224 * j + LANES)
        last = tail[48:]
        spread = jnp.concatenate([pltpu.roll(last, 96 - 32 * q, 1) for q in range(3)], axis=0)
        out_ref[0, j, :64, :] = main.astype(jnp.bfloat16)
        out_ref[0, j, 64:, :] = jnp.where(lane < 96, tail[:48], spread).astype(jnp.bfloat16)


def pack(gate_master, up_master, gain):
    experts, rows, cols = gate_master.shape
    return pl.pallas_call(
        pack_kernel,
        grid=(experts,),
        in_specs=[
            pl.BlockSpec((1, rows, cols), lambda i: (i, 0, 0)),
            pl.BlockSpec((1, rows, cols), lambda i: (i, 0, 0)),
            pl.BlockSpec((rows, 1), lambda i: (0, 0)),
        ],
        out_specs=pl.BlockSpec((1, 4, 112, LANES), lambda i: (i, 0, 0, 0)),
        out_shape=jax.ShapeDtypeStruct((experts, 4, 112, LANES), jnp.bfloat16),
        cost_estimate=pl.CostEstimate(flops=4000000, bytes_accessed=2800000, transcendentals=0),
        compiler_params=pltpu.CompilerParams(vmem_limit_bytes=4 * 2**20),
        name="pack",
    )(gate_master, up_master, gain)


def unpack_kernel(tiles_ref, gate_ref, up_ref):
    lane = lax.broadcasted_iota(jnp.int32, (16, LANES), 1)
    for s in range(tiles_ref.shape[0]):
        rows = pl.ds(32 * s, 32)
        gate_ref[0, rows, :LANES] = tiles_ref[s, 0:32, :]
        up_ref[0, rows, :LANES] = tiles_ref[s, 32:64, :]
        gate_ref[0, rows, LANES:] = tiles_ref[s, 64:96, :96]
        up_ref[0, pl.ds(32 * s, 16), LANES:] = tiles_ref[s, 96:112, :96]
        parts = [
            pltpu.roll(
                tiles_ref[s, 64 + 16 * q : 80 + 16 * q, :].astype(jnp.float32), 32 * q + 32, 1
            )
            for q in range(3)
        ]
        last = jnp.where(lane < 32, parts[0], jnp.where(lane < 64, parts[1], parts[2]))
        up_ref[0, pl.ds(32 * s + 16, 16), LANES:] = last[:, :96].astype(jnp.bfloat16)


def unpack(tiles):
    count = tiles.shape[0]
    step = 16
    out = jax.ShapeDtypeStruct((1, 32 * count, 224), jnp.bfloat16)
    return pl.pallas_call(
        unpack_kernel,
        grid=(count // step,),
        in_specs=[pl.BlockSpec((step, 112, LANES), lambda i: (i, 0, 0))],
        out_specs=[pl.BlockSpec((1, 32 * step, 224), lambda i: (0, i, 0))] * 2,
        out_shape=[out, out],
        cost_estimate=pl.CostEstimate(flops=2000000, bytes_accessed=3800000, transcendentals=0),
        compiler_params=pltpu.CompilerParams(vmem_limit_bytes=6 * 2**20),
        name="unpack",
    )(tiles)


def permutation(sizes, move):
    groups, fs_0, fs_1, tp = sizes
    pairs = []
    for g in range(groups):
        for a in range(fs_0):
            for b in range(fs_1):
                for t in range(tp):
                    z, y = move(g * fs_0 + a, b, t)
                    z, y = z % (groups * fs_0), y % fs_1
                    pairs.append((((g * fs_0 + a) * fs_1 + b) * tp + t, (z * fs_1 + y) * tp + t))
    return pairs


def local(sizes, tokens, route_ids, route_logits, norm_gain, gate_master, up_master, down_master):
    f32, bf16 = jnp.float32, jnp.bfloat16
    fs_1, tp_size = sizes[2], sizes[3]

    def along_z(x, hops):
        pairs = permutation(sizes, lambda z, y, t: (z + (hops if t % 2 == 0 else -hops), y))
        return lax.ppermute(x, ALL, pairs)

    def along_y(x, hops):
        return lax.ppermute(x, ALL, permutation(sizes, lambda z, y, t: (z, y + hops)))

    as_float = tokens.astype(f32)
    normed = (
        as_float * lax.rsqrt(jnp.mean(as_float * as_float, axis=-1, keepdims=True) + EPS)
    ).astype(bf16)
    differ = route_logits[:, 0] - route_logits[:, 1]
    route_weight = jnp.stack([jax.nn.sigmoid(differ), jax.nn.sigmoid(-differ)], axis=1)
    expert_ids = jnp.arange(tp_size, dtype=jnp.int32)
    route_hits = route_ids[None, :, :] == expert_ids[:, None, None]
    chosen = jnp.any(route_hits, axis=2)
    slot_rank = jnp.cumsum(chosen.astype(jnp.int32), axis=1) - 1
    slot_ids = jnp.arange(CAP, dtype=jnp.int32)
    picker = chosen[:, None, :] & (slot_rank[:, None, :] == slot_ids[None, :, None])
    weight_rows = jnp.sum(jnp.where(route_hits, route_weight[None, :, :], 0.0), axis=2)
    mine = lax.axis_index("tp")
    my_picker = lax.dynamic_index_in_dim(picker, mine, 0, keepdims=False)
    my_weights = lax.dynamic_index_in_dim(weight_rows, mine, 0, keepdims=False)
    slot_weight = jnp.sum(jnp.where(my_picker, my_weights[None, :], 0.0), axis=1)
    packed = jnp.dot(my_picker.astype(bf16), normed, preferred_element_type=f32).astype(bf16)

    down_half = down_master.astype(bf16)
    down_tiles = lax.all_to_all(down_half, "tp", 0, 0, tiled=True)
    down_own = jnp.moveaxis(down_tiles, 0, 1).reshape(down_tiles.shape[1], -1)
    across = permutation(sizes, lambda z, y, t: (z + sizes[1], y))
    down_other = lax.ppermute(down_own, ALL, across)

    tiles = pack(gate_master, up_master, norm_gain[:, None])
    tiles = lax.all_to_all(tiles, "tp", 0, 0, tiled=True).reshape(-1, 112, LANES)
    tiles = jnp.concatenate([tiles, tiles], axis=0)
    tiles = lax.all_to_all(tiles, GR_FS, 0, 0, tiled=True)

    held = packed
    for hops in (4, 2, 1):
        moved = along_z(held, hops)
        held = jnp.concatenate([held, moved], axis=0)
    row = lax.axis_index("fs_1")
    gathered = jnp.zeros((fs_1, *held.shape), bf16)
    for k in range(fs_1):
        moved = held
        if k:
            moved = along_y(held, k)
        gathered = lax.dynamic_update_index_in_dim(gathered, moved, (row + fs_1 - k) % fs_1, 0)
    gathered = gathered.reshape(-1, gathered.shape[2])
    tiles, gathered, down_other = lax.optimization_barrier((tiles, gathered, down_other))

    gate_weight, up_weight = unpack(tiles)
    low = lax.axis_index("gr") == 0
    down_parts = [jnp.where(low, down_own, down_other), jnp.where(low, down_other, down_own)]
    down_weight = jnp.concatenate(down_parts, axis=1)[None]

    gate_act = jnp.dot(gathered, gate_weight[0], preferred_element_type=f32)
    up_act = jnp.dot(gathered, up_weight[0], preferred_element_type=f32)
    hidden = (jax.nn.silu(gate_act) * up_act).astype(bf16)
    everyone = picker.reshape(-1, picker.shape[2]).astype(bf16)
    mixed = []
    for part in down_parts:
        sums = jnp.dot(hidden, part, preferred_element_type=f32).astype(bf16)
        sums = lax.all_to_all(sums.reshape(fs_1, -1, sums.shape[1]), "fs_1", 0, 0, tiled=True)
        total = jnp.sum(sums.astype(f32), axis=0)
        for hops in (1, 2, 4):
            half = total.shape[0] // 2
            moved = along_z(total[half:].astype(bf16), -hops)
            total = total[:half] + moved.astype(f32)
        block = (total * slot_weight[:, None]).astype(bf16)
        block, slot_weight = lax.optimization_barrier((block, slot_weight))
        blocks = lax.all_to_all(
            jnp.broadcast_to(block[None], (tp_size, *block.shape)), "tp", 0, 0, tiled=True
        )
        mixed.append(
            lax.dot_general(
                everyone,
                blocks.reshape(-1, blocks.shape[2]),
                (((0,), (0,)), ((), ())),
                preferred_element_type=f32,
            ).astype(bf16)
        )
    return (gate_weight, up_weight, down_weight, jnp.concatenate(mixed, axis=1))


def solution(mesh):
    sizes = (mesh.shape["gr"], 8, 4, mesh.shape["tp"])
    torus = Mesh(mesh.devices.reshape(sizes), ALL)
    in_specs = (
        P(GR_FS, None),
        P(GR_FS, None),
        P(GR_FS, None),
        P(GR_FS),
        P(None, GR_FS, "tp"),
        P(None, GR_FS, "tp"),
        P(None, FS, ("gr", "tp")),
    )
    out_specs = (P("tp", None, FS), P("tp", None, FS), P("tp", FS, None), P(GR_FS, None))

    def call(*arrays):
        return local(sizes, *arrays)

    return jax.shard_map(call, mesh=torus, in_specs=in_specs, out_specs=out_specs, check_vma=False)
```

```python
import jax
import jax.numpy as jnp
from jax import lax
from jax.experimental import pallas as pl
from jax.experimental.pallas import tpu as pltpu
from jax.sharding import Mesh
from jax.sharding import PartitionSpec as P


CAP = 32
FS = ("fs_0", "fs_1")
GR_FS = ("gr", "fs_0", "fs_1")
ALL = ("gr", "fs_0", "fs_1", "tp")
EPS = 1e-06
LANES = 128


def lane_window(blocks, start):
    first, offset = divmod(start, LANES)
    if offset == 0:
        return blocks[first]
    head = pltpu.roll(blocks[first], LANES - offset, 1)
    if first + 1 == len(blocks):
        return head
    rest = pltpu.roll(blocks[first + 1], LANES - offset, 1)
    lane = lax.broadcasted_iota(jnp.int32, head.shape, 1)
    return jnp.where(lane < LANES - offset, head, rest)


def pack_kernel(gate_ref, up_ref, gain_ref, out_ref):
    gain = gain_ref[...]
    both = jnp.concatenate([gate_ref[0] * gain, up_ref[0] * gain], axis=0)
    blocks = [both[:, LANES * b : LANES * (b + 1)] for b in range(both.shape[1] // LANES)]
    lane = lax.broadcasted_iota(jnp.int32, (48, LANES), 1)
    for j in range(4):
        main = lane_window(blocks, 224 * j)
        tail = lane_window(blocks, 224 * j + LANES)
        last = tail[48:]
        spread = jnp.concatenate([pltpu.roll(last, 96 - 32 * q, 1) for q in range(3)], axis=0)
        out_ref[0, 112 * j : 112 * j + 64, :] = main.astype(jnp.bfloat16)
        out_ref[0, 112 * j + 64 : 112 * j + 112, :] = jnp.where(lane < 96, tail[:48], spread).astype(jnp.bfloat16)


def pack(gate_master, up_master, gain):
    experts, rows, cols = gate_master.shape
    return pl.pallas_call(
        pack_kernel,
        grid=(experts,),
        in_specs=[
            pl.BlockSpec((1, rows, cols), lambda i: (i, 0, 0)),
            pl.BlockSpec((1, rows, cols), lambda i: (i, 0, 0)),
            pl.BlockSpec((rows, 1), lambda i: (0, 0)),
        ],
        out_specs=pl.BlockSpec((1, 448, LANES), lambda i: (i, 0, 0)),
        out_shape=jax.ShapeDtypeStruct((experts, 448, LANES), jnp.bfloat16),
        cost_estimate=pl.CostEstimate(flops=4000000, bytes_accessed=2800000, transcendentals=0),
        compiler_params=pltpu.CompilerParams(vmem_limit_bytes=4 * 2**20),
        name="pack",
    )(gate_master, up_master, gain)


def unpack_kernel(tiles_ref, gate_ref, up_ref):
    lane = lax.broadcasted_iota(jnp.int32, (16, LANES), 1)
    for s in range(tiles_ref.shape[0]):
        rows = pl.ds(32 * s, 32)
        gate_ref[0, rows, :LANES] = tiles_ref[s, 0:32, :]
        up_ref[0, rows, :LANES] = tiles_ref[s, 32:64, :]
        gate_ref[0, rows, LANES:] = tiles_ref[s, 64:96, :96]
        up_ref[0, pl.ds(32 * s, 16), LANES:] = tiles_ref[s, 96:112, :96]
        parts = [
            pltpu.roll(
                tiles_ref[s, 64 + 16 * q : 80 + 16 * q, :].astype(jnp.float32), 32 * q + 32, 1
            )
            for q in range(3)
        ]
        last = jnp.where(lane < 32, parts[0], jnp.where(lane < 64, parts[1], parts[2]))
        up_ref[0, pl.ds(32 * s + 16, 16), LANES:] = last[:, :96].astype(jnp.bfloat16)


def unpack(tiles):
    count = tiles.shape[0]
    step = 16
    out = jax.ShapeDtypeStruct((1, 32 * count, 224), jnp.bfloat16)
    return pl.pallas_call(
        unpack_kernel,
        grid=(count // step,),
        in_specs=[pl.BlockSpec((step, 112, LANES), lambda i: (i, 0, 0))],
        out_specs=[pl.BlockSpec((1, 32 * step, 224), lambda i: (0, i, 0))] * 2,
        out_shape=[out, out],
        cost_estimate=pl.CostEstimate(flops=2000000, bytes_accessed=3800000, transcendentals=0),
        compiler_params=pltpu.CompilerParams(vmem_limit_bytes=6 * 2**20),
        name="unpack",
    )(tiles)


def permutation(sizes, move):
    groups, fs_0, fs_1, tp = sizes
    pairs = []
    for g in range(groups):
        for a in range(fs_0):
            for b in range(fs_1):
                for t in range(tp):
                    z, y = move(g * fs_0 + a, b, t)
                    z, y = z % (groups * fs_0), y % fs_1
                    pairs.append((((g * fs_0 + a) * fs_1 + b) * tp + t, (z * fs_1 + y) * tp + t))
    return pairs


def local(sizes, tokens, route_ids, route_logits, norm_gain, gate_master, up_master, down_master):
    f32, bf16 = jnp.float32, jnp.bfloat16
    fs_1, tp_size = sizes[2], sizes[3]

    def along_z(x, hops):
        pairs = permutation(sizes, lambda z, y, t: (z + (hops if t % 2 == 0 else -hops), y))
        return lax.ppermute(x, ALL, pairs)

    def along_y(x, hops):
        return lax.ppermute(x, ALL, permutation(sizes, lambda z, y, t: (z, y + hops)))

    as_float = tokens.astype(f32)
    normed = (
        as_float * lax.rsqrt(jnp.mean(as_float * as_float, axis=-1, keepdims=True) + EPS)
    ).astype(bf16)
    differ = route_logits[:, 0] - route_logits[:, 1]
    route_weight = jnp.stack([jax.nn.sigmoid(differ), jax.nn.sigmoid(-differ)], axis=1)
    expert_ids = jnp.arange(tp_size, dtype=jnp.int32)
    route_hits = route_ids[None, :, :] == expert_ids[:, None, None]
    chosen = jnp.any(route_hits, axis=2)
    slot_rank = jnp.cumsum(chosen.astype(jnp.int32), axis=1) - 1
    slot_ids = jnp.arange(CAP, dtype=jnp.int32)
    picker = chosen[:, None, :] & (slot_rank[:, None, :] == slot_ids[None, :, None])
    weight_rows = jnp.sum(jnp.where(route_hits, route_weight[None, :, :], 0.0), axis=2)
    mine = lax.axis_index("tp")
    my_picker = lax.dynamic_index_in_dim(picker, mine, 0, keepdims=False)
    slot_weight = jnp.sum(jnp.where(picker, weight_rows[:, None, :], 0.0), axis=2)
    packed = jnp.dot(my_picker.astype(bf16), normed, preferred_element_type=f32).astype(bf16)

    down_tiles = down_master.astype(bf16)
    down_tiles = lax.all_to_all(down_tiles, "tp", 0, 0, tiled=True)
    down_own = jnp.moveaxis(down_tiles, 0, 1).reshape(down_tiles.shape[1], -1)
    across = permutation(sizes, lambda z, y, t: (z + sizes[1], y))
    down_other = lax.ppermute(down_own, ALL, across)

    tiles = pack(gate_master, up_master, norm_gain[:, None])
    tiles = lax.all_to_all(tiles, "tp", 0, 0, tiled=True).reshape(-1, 112, LANES)
    tiles = jnp.concatenate([tiles, tiles], axis=0)
    tiles = lax.all_to_all(tiles, GR_FS, 0, 0, tiled=True)

    held = packed
    for hops in (4, 2, 1):
        moved = along_z(held, hops)
        held = jnp.concatenate([held, moved], axis=0)
    row = lax.axis_index("fs_1")
    gathered = jnp.zeros((fs_1, *held.shape), bf16)
    for k in range(fs_1):
        moved = held
        if k:
            moved = along_y(held, k)
        gathered = lax.dynamic_update_index_in_dim(gathered, moved, (row + fs_1 - k) % fs_1, 0)
    gathered = gathered.reshape(-1, gathered.shape[2])
    low = lax.axis_index("gr") == 0
    down_weight = jnp.concatenate(
        [jnp.where(low, down_own, down_other), jnp.where(low, down_other, down_own)], axis=1
    )
    columns = down_weight.shape[1] // fs_1
    down_cols = []
    for k in range(fs_1):
        picked = lax.dynamic_slice_in_dim(down_weight, (row + k) % fs_1 * columns, columns, axis=1)
        if k:
            picked = along_y(picked, k)
        down_cols.append(picked)
    tiles, gathered = lax.optimization_barrier((tiles, gathered))
    gate_weight, up_weight = unpack(tiles)

    gate_act = jnp.dot(gathered, gate_weight[0], preferred_element_type=f32)
    up_act = jnp.dot(gathered, up_weight[0], preferred_element_type=f32)
    hidden = (jax.nn.silu(gate_act) * up_act).astype(bf16)
    hidden = hidden.reshape(fs_1, -1, hidden.shape[1])
    half = hidden.shape[1] // 2

    def over_hidden(part):
        total = 0.0
        for k in range(fs_1):
            moved = part
            if k:
                moved = along_y(part, k)
            total = total + jnp.dot(
                moved.reshape(-1, moved.shape[2]), down_cols[k], preferred_element_type=f32
            )
        return total.reshape(fs_1, -1, columns)

    odd = over_hidden(hidden[:, half:])
    total = over_hidden(hidden[:, :half])
    for hops in (1, 2, 4):
        moved = along_z(odd.astype(bf16), -hops)
        total = total + moved.astype(f32)
        half = total.shape[1] // 2
        total, odd = total[:, :half], total[:, half:]
        if hops == 4:
            total = jnp.concatenate([total, odd], axis=1)

    block = total.astype(bf16)
    block = jnp.broadcast_to(block[:, None], (fs_1, tp_size, *block.shape[1:]))
    blocks = lax.all_to_all(block.reshape(-1, *block.shape[2:]), ("fs_1", "tp"), 0, 0, tiled=True)
    blocks = blocks.reshape(fs_1, -1, columns).astype(f32) * slot_weight.reshape(1, -1, 1)
    blocks = jnp.moveaxis(blocks.astype(bf16), 0, 1).reshape(-1, fs_1 * columns)
    mixed = lax.dot_general(
        picker.reshape(-1, picker.shape[2]).astype(bf16),
        blocks,
        (((0,), (0,)), ((), ())),
        preferred_element_type=f32,
    ).astype(bf16)
    return (gate_weight, up_weight, down_weight[None], mixed)


def solution(mesh):
    sizes = (mesh.shape["gr"], 8, 4, mesh.shape["tp"])
    torus = Mesh(mesh.devices.reshape(sizes), ALL)
    in_specs = (
        P(GR_FS, None),
        P(GR_FS, None),
        P(GR_FS, None),
        P(GR_FS),
        P(None, GR_FS, "tp"),
        P(None, GR_FS, "tp"),
        P(None, FS, ("gr", "tp")),
    )
    out_specs = (P("tp", None, FS), P("tp", None, FS), P("tp", FS, None), P(GR_FS, None))

    def call(*arrays):
        return local(sizes, *arrays)

    return jax.shard_map(call, mesh=torus, in_specs=in_specs, out_specs=out_specs, check_vma=False)
```

```python
import jax
import jax.numpy as jnp
from jax import lax
from jax.experimental import pallas as pl
from jax.experimental.pallas import tpu as pltpu
from jax.sharding import Mesh
from jax.sharding import PartitionSpec as P


CAP = 32
FS = ("fs_0", "fs_1")
GR_FS = ("gr", "fs_0", "fs_1")
ALL = ("gr", "fs_0", "fs_1", "tp")
EPS = 1e-06
LANES = 128


def lane_window(blocks, start):
    first, offset = divmod(start, LANES)
    if offset == 0:
        return blocks[first]
    head = pltpu.roll(blocks[first], LANES - offset, 1)
    if first + 1 == len(blocks):
        return head
    rest = pltpu.roll(blocks[first + 1], LANES - offset, 1)
    lane = lax.broadcasted_iota(jnp.int32, head.shape, 1)
    return jnp.where(lane < LANES - offset, head, rest)


def pack_kernel(gate_ref, up_ref, gain_ref, out_ref):
    gain = gain_ref[...]
    both = jnp.concatenate([gate_ref[0] * gain, up_ref[0] * gain], axis=0)
    blocks = [both[:, LANES * b : LANES * (b + 1)] for b in range(both.shape[1] // LANES)]
    lane = lax.broadcasted_iota(jnp.int32, (48, LANES), 1)
    for j in range(4):
        main = lane_window(blocks, 224 * j)
        tail = lane_window(blocks, 224 * j + LANES)
        last = tail[48:]
        spread = jnp.concatenate([pltpu.roll(last, 96 - 32 * q, 1) for q in range(3)], axis=0)
        out_ref[0, 112 * j : 112 * j + 64, :] = main.astype(jnp.bfloat16)
        out_ref[0, 112 * j + 64 : 112 * j + 112, :] = jnp.where(lane < 96, tail[:48], spread).astype(jnp.bfloat16)


def pack(gate_master, up_master, gain):
    experts, rows, cols = gate_master.shape
    return pl.pallas_call(
        pack_kernel,
        grid=(experts,),
        in_specs=[
            pl.BlockSpec((1, rows, cols), lambda i: (i, 0, 0)),
            pl.BlockSpec((1, rows, cols), lambda i: (i, 0, 0)),
            pl.BlockSpec((rows, 1), lambda i: (0, 0)),
        ],
        out_specs=pl.BlockSpec((1, 448, LANES), lambda i: (i, 0, 0)),
        out_shape=jax.ShapeDtypeStruct((experts, 448, LANES), jnp.bfloat16),
        cost_estimate=pl.CostEstimate(flops=4000000, bytes_accessed=2800000, transcendentals=0),
        compiler_params=pltpu.CompilerParams(vmem_limit_bytes=58 * 2**20),
        name="pack",
    )(gate_master, up_master, gain)


def hidden_kernel(tiles_ref, tokens_ref, gate_ref, up_ref, even_ref, odd_ref):
    @pl.when(pl.program_id(0) == 0)
    def _():
        lane = lax.broadcasted_iota(jnp.int32, (16, LANES), 1)

        def unpack(s, carry):
            rows = pl.ds(pl.multiple_of(32 * s, 32), 32)
            gate_ref[0, rows, :LANES] = tiles_ref[s, 0:32, :]
            up_ref[0, rows, :LANES] = tiles_ref[s, 32:64, :]
            gate_ref[0, rows, LANES:] = tiles_ref[s, 64:96, :96]
            up_ref[0, pl.ds(pl.multiple_of(32 * s, 16), 16), LANES:] = tiles_ref[s, 96:112, :96]
            parts = [
                pltpu.roll(
                    tiles_ref[s, 64 + 16 * q : 80 + 16 * q, :].astype(jnp.float32), 32 * q + 32, 1
                )
                for q in range(3)
            ]
            last = jnp.where(lane < 32, parts[0], jnp.where(lane < 64, parts[1], parts[2]))
            rest = pl.ds(pl.multiple_of(32 * s + 16, 16), 16)
            up_ref[0, rest, LANES:] = last[:, :96].astype(jnp.bfloat16)
            return carry

        lax.fori_loop(0, tiles_ref.shape[0], unpack, 0, unroll=4)

    tokens = tokens_ref[...]
    gate = jnp.dot(tokens, gate_ref[0], preferred_element_type=jnp.float32)
    up = jnp.dot(tokens, up_ref[0], preferred_element_type=jnp.float32)
    hidden = (gate / (1.0 + jnp.exp(-gate)) * up).astype(jnp.bfloat16)
    half = hidden.shape[0] // 2
    even_ref[0] = hidden[:half]
    for k in range(odd_ref.shape[0]):
        odd_ref[k, 0, :, :224] = hidden[half:]
        odd_ref[k, 0, :, 224:] = jnp.zeros((half, 32), jnp.bfloat16)


def hidden_units(tiles, tokens, pieces):
    count = tiles.shape[0]
    rows = tokens.shape[0] // pieces
    weight = jax.ShapeDtypeStruct((1, 32 * count, 224), jnp.bfloat16)
    even = jax.ShapeDtypeStruct((pieces, rows // 2, 224), jnp.bfloat16)
    odd = jax.ShapeDtypeStruct((pieces, pieces, rows // 2, 256), jnp.bfloat16)
    return pl.pallas_call(
        hidden_kernel,
        grid=(pieces,),
        in_specs=[
            pl.BlockSpec(tiles.shape, lambda i: (0, 0, 0)),
            pl.BlockSpec((rows, tokens.shape[1]), lambda i: (i, 0)),
        ],
        out_specs=[pl.BlockSpec(weight.shape, lambda i: (0, 0, 0))] * 2
        + [
            pl.BlockSpec((1, rows // 2, 224), lambda i: (i, 0, 0)),
            pl.BlockSpec((pieces, 1, rows // 2, 256), lambda i: (0, i, 0, 0)),
        ],
        out_shape=[weight, weight, even, odd],
        cost_estimate=pl.CostEstimate(
            flops=1900000000, bytes_accessed=8500000, transcendentals=230000
        ),
        compiler_params=pltpu.CompilerParams(
            dimension_semantics=("arbitrary",), vmem_limit_bytes=58 * 2**20
        ),
        name="hidden_units",
    )(tiles, tokens)


def out_kernel(*refs):
    out_ref = refs[-1]
    count = (len(refs) - 1) // 2
    for i in range(out_ref.shape[0]):
        total = jnp.dot(refs[0][i], refs[count][...], preferred_element_type=jnp.float32)
        for k in range(1, count):
            total = total + jnp.dot(
                refs[k][i], refs[count + k][...], preferred_element_type=jnp.float32
            )
        out_ref[i] = total.astype(out_ref.dtype)


def all_out_kernel(row_ref, hidden_ref, *refs):
    out_ref = refs[-1]
    count = hidden_ref.shape[0]
    for i in range(out_ref.shape[0]):
        total = jnp.dot(
            hidden_ref[row_ref[0], i, :, :224], refs[0][...], preferred_element_type=jnp.float32
        )
        for k in range(1, count):
            source = lax.rem(row_ref[0] + (count - k), count)
            total = total + jnp.dot(
                hidden_ref[source, i, :, :224], refs[k][...], preferred_element_type=jnp.float32
            )
        out_ref[i] = total.astype(out_ref.dtype)


def partial_out(hidden, down, kind, row=None):
    shape = (*hidden[0].shape[-3:-1], down[0].shape[1])
    whole = pl.BlockSpec(memory_space=pltpu.VMEM)
    first = [] if row is None else [row]
    return pl.pallas_call(
        out_kernel if row is None else all_out_kernel,
        in_specs=[pl.BlockSpec(memory_space=pltpu.SMEM)] * len(first)
        + [whole] * (len(hidden) + len(down)),
        out_specs=whole,
        out_shape=jax.ShapeDtypeStruct(shape, kind),
        cost_estimate=pl.CostEstimate(
            flops=470000000, bytes_accessed=3000000, transcendentals=0
        ),
        compiler_params=pltpu.CompilerParams(vmem_limit_bytes=12 * 2**20),
        name="partial_out",
    )(*first, *hidden, *down)


def permutation(sizes, move):
    groups, fs_0, fs_1, tp = sizes
    pairs = []
    for g in range(groups):
        for a in range(fs_0):
            for b in range(fs_1):
                for t in range(tp):
                    z, y = move(g * fs_0 + a, b, t)
                    z, y = z % (groups * fs_0), y % fs_1
                    pairs.append((((g * fs_0 + a) * fs_1 + b) * tp + t, (z * fs_1 + y) * tp + t))
    return pairs


def local(sizes, tokens, route_ids, route_logits, norm_gain, gate_master, up_master, down_master):
    f32, bf16 = jnp.float32, jnp.bfloat16
    fs_1, tp_size = sizes[2], sizes[3]

    def along_z(x, hops):
        pairs = permutation(sizes, lambda z, y, t: (z + (hops if t % 2 == 0 else -hops), y))
        return lax.ppermute(x, ALL, pairs)

    def along_y(x, hops):
        return lax.ppermute(x, ALL, permutation(sizes, lambda z, y, t: (z, y + hops)))

    as_float = tokens.astype(f32)
    normed = (
        as_float * lax.rsqrt(jnp.mean(as_float * as_float, axis=-1, keepdims=True) + EPS)
    ).astype(bf16)
    differ = route_logits[:, 0] - route_logits[:, 1]
    route_weight = jnp.stack([jax.nn.sigmoid(differ), jax.nn.sigmoid(-differ)], axis=1)
    expert_ids = jnp.arange(tp_size, dtype=jnp.int32)
    route_hits = route_ids[None, :, :] == expert_ids[:, None, None]
    chosen = jnp.any(route_hits, axis=2)
    slot_rank = jnp.cumsum(chosen.astype(jnp.int32), axis=1) - 1
    slot_ids = jnp.arange(CAP, dtype=jnp.int32)
    picker = chosen[:, None, :] & (slot_rank[:, None, :] == slot_ids[None, :, None])
    weight_rows = jnp.sum(jnp.where(route_hits, route_weight[None, :, :], 0.0), axis=2)
    mine = lax.axis_index("tp")
    my_picker = lax.dynamic_index_in_dim(picker, mine, 0, keepdims=False)
    slot_weight = jnp.sum(jnp.where(picker, weight_rows[:, None, :], 0.0), axis=2)
    packed = jnp.dot(my_picker.astype(bf16), normed, preferred_element_type=f32).astype(bf16)

    down_tiles = down_master.astype(bf16)
    down_tiles = lax.all_to_all(down_tiles, "tp", 0, 0, tiled=True)
    down_own = jnp.moveaxis(down_tiles, 0, 1).reshape(down_tiles.shape[1], -1)
    across = permutation(sizes, lambda z, y, t: (z + sizes[1], y))
    down_other = lax.ppermute(down_own, ALL, across)

    tiles = pack(gate_master, up_master, norm_gain[:, None])
    tiles = lax.all_to_all(tiles, "tp", 0, 0, tiled=True).reshape(-1, 112, LANES)
    tiles = jnp.concatenate([tiles, tiles], axis=0)
    tiles = lax.all_to_all(tiles, GR_FS, 0, 0, tiled=True)

    held = packed
    for hops in (4, 2, 1):
        moved = along_z(held, hops)
        held = jnp.concatenate([held, moved], axis=0)
    row = lax.axis_index("fs_1")
    gathered = jnp.zeros((fs_1, *held.shape), bf16)
    for k in range(fs_1):
        moved = held
        if k:
            moved = along_y(held, k)
        gathered = lax.dynamic_update_index_in_dim(gathered, moved, (row + fs_1 - k) % fs_1, 0)
    gathered = gathered.reshape(-1, gathered.shape[2])
    low = lax.axis_index("gr") == 0
    down_weight = jnp.concatenate(
        [jnp.where(low, down_own, down_other), jnp.where(low, down_other, down_own)], axis=1
    )
    columns = down_weight.shape[1] // fs_1
    down_cols = []
    for k in range(fs_1):
        picked = lax.dynamic_slice_in_dim(down_weight, (row + k) % fs_1 * columns, columns, axis=1)
        if k:
            picked = along_y(picked, k)
        down_cols.append(picked)
    tiles, gathered = lax.optimization_barrier((tiles, gathered))
    gate_weight, up_weight, even, odd = hidden_units(tiles, gathered, fs_1)

    odd = lax.all_to_all(odd, "fs_1", 0, 0, tiled=True)
    pieces = [even]
    for k in range(1, fs_1):
        pieces.append(along_y(even, k))
    odd = partial_out([odd], down_cols, bf16, row.astype(jnp.int32)[None])
    total = partial_out(pieces, down_cols, f32)
    for hops in (1, 2, 4):
        moved = along_z(odd.astype(bf16), -hops)
        total = total + moved.astype(f32)
        half = total.shape[1] // 2
        total, odd = total[:, :half], total[:, half:]
        if hops == 4:
            total = jnp.concatenate([total, odd], axis=1)

    block = total.astype(bf16)
    block = jnp.broadcast_to(block[:, None], (fs_1, tp_size, *block.shape[1:]))
    blocks = lax.all_to_all(block.reshape(-1, *block.shape[2:]), ("fs_1", "tp"), 0, 0, tiled=True)
    blocks = blocks.reshape(fs_1, -1, columns).astype(f32) * slot_weight.reshape(1, -1, 1)
    blocks = jnp.moveaxis(blocks.astype(bf16), 0, 1).reshape(-1, fs_1 * columns)
    mixed = lax.dot_general(
        picker.reshape(-1, picker.shape[2]).astype(bf16),
        blocks,
        (((0,), (0,)), ((), ())),
        preferred_element_type=f32,
    ).astype(bf16)
    return (gate_weight, up_weight, down_weight[None], mixed)


def solution(mesh):
    sizes = (mesh.shape["gr"], 8, 4, mesh.shape["tp"])
    torus = Mesh(mesh.devices.reshape(sizes), ALL)
    in_specs = (
        P(GR_FS, None),
        P(GR_FS, None),
        P(GR_FS, None),
        P(GR_FS),
        P(None, GR_FS, "tp"),
        P(None, GR_FS, "tp"),
        P(None, FS, ("gr", "tp")),
    )
    out_specs = (P("tp", None, FS), P("tp", None, FS), P("tp", FS, None), P(GR_FS, None))

    def call(*arrays):
        return local(sizes, *arrays)

    return jax.shard_map(call, mesh=torus, in_specs=in_specs, out_specs=out_specs, check_vma=False)
```

```python
import jax
import jax.numpy as jnp
from jax import lax
from jax.experimental import pallas as pl
from jax.experimental.pallas import tpu as pltpu
from jax.sharding import Mesh
from jax.sharding import PartitionSpec as P


CAP = 32
FS = ("fs_0", "fs_1")
GR_FS = ("gr", "fs_0", "fs_1")
ALL = ("gr", "fs_0", "fs_1", "tp")
EPS = 1e-06
LANES = 128


def lane_window(blocks, start):
    first, offset = divmod(start, LANES)
    if offset == 0:
        return blocks[first]
    head = pltpu.roll(blocks[first], LANES - offset, 1)
    if first + 1 == len(blocks):
        return head
    rest = pltpu.roll(blocks[first + 1], LANES - offset, 1)
    lane = lax.broadcasted_iota(jnp.int32, head.shape, 1)
    return jnp.where(lane < LANES - offset, head, rest)


def pack_kernel(gate_ref, up_ref, gain_ref, out_ref):
    gain = gain_ref[...]
    both = jnp.concatenate([gate_ref[0] * gain, up_ref[0] * gain], axis=0)
    blocks = [both[:, LANES * b : LANES * (b + 1)] for b in range(both.shape[1] // LANES)]
    lane = lax.broadcasted_iota(jnp.int32, (48, LANES), 1)
    for j in range(4):
        main = lane_window(blocks, 224 * j)
        tail = lane_window(blocks, 224 * j + LANES)
        last = tail[48:]
        spread = jnp.concatenate([pltpu.roll(last, 96 - 32 * q, 1) for q in range(3)], axis=0)
        out_ref[0, 112 * j : 112 * j + 64, :] = main.astype(jnp.bfloat16)
        out_ref[0, 112 * j + 64 : 112 * j + 112, :] = jnp.where(lane < 96, tail[:48], spread).astype(jnp.bfloat16)


def pack(gate_master, up_master, gain):
    experts, rows, cols = gate_master.shape
    return pl.pallas_call(
        pack_kernel,
        grid=(experts,),
        in_specs=[
            pl.BlockSpec((1, rows, cols), lambda i: (i, 0, 0)),
            pl.BlockSpec((1, rows, cols), lambda i: (i, 0, 0)),
            pl.BlockSpec((rows, 1), lambda i: (0, 0)),
        ],
        out_specs=pl.BlockSpec((1, 448, LANES), lambda i: (i, 0, 0)),
        out_shape=jax.ShapeDtypeStruct((experts, 448, LANES), jnp.bfloat16),
        cost_estimate=pl.CostEstimate(flops=4000000, bytes_accessed=2800000, transcendentals=0),
        compiler_params=pltpu.CompilerParams(vmem_limit_bytes=58 * 2**20),
        name="pack",
    )(gate_master, up_master, gain)


def hidden_kernel(tiles_ref, tokens_ref, gate_ref, up_ref, even_ref, odd_ref):
    @pl.when(pl.program_id(0) == 0)
    def _():
        lane = lax.broadcasted_iota(jnp.int32, (16, LANES), 1)

        for s in range(tiles_ref.shape[0]):
            rows = pl.ds(32 * s, 32)
            gate_ref[0, rows, :LANES] = tiles_ref[s, 0:32, :]
            up_ref[0, rows, :LANES] = tiles_ref[s, 32:64, :]
            gate_ref[0, rows, LANES:] = tiles_ref[s, 64:96, :96]
            up_ref[0, pl.ds(32 * s, 16), LANES:] = tiles_ref[s, 96:112, :96]
            parts = [
                pltpu.roll(
                    tiles_ref[s, 64 + 16 * q : 80 + 16 * q, :].astype(jnp.float32), 32 * q + 32, 1
                )
                for q in range(3)
            ]
            last = jnp.where(lane < 32, parts[0], jnp.where(lane < 64, parts[1], parts[2]))
            up_ref[0, pl.ds(32 * s + 16, 16), LANES:] = last[:, :96].astype(jnp.bfloat16)

    tokens = tokens_ref[...]
    gate = jnp.dot(tokens, gate_ref[0], preferred_element_type=jnp.float32)
    up = jnp.dot(tokens, up_ref[0], preferred_element_type=jnp.float32)
    hidden = (gate / (1.0 + jnp.exp(-gate)) * up).astype(jnp.bfloat16)
    half = hidden.shape[0] // 2
    even_ref[0] = hidden[:half]
    for k in range(odd_ref.shape[0]):
        odd_ref[k, 0, :, :224] = hidden[half:]
        odd_ref[k, 0, :, 224:] = jnp.zeros((half, 32), jnp.bfloat16)


def hidden_units(tiles, tokens, pieces):
    count = tiles.shape[0]
    rows = tokens.shape[0] // pieces
    weight = jax.ShapeDtypeStruct((1, 32 * count, 224), jnp.bfloat16)
    even = jax.ShapeDtypeStruct((pieces, rows // 2, 224), jnp.bfloat16)
    odd = jax.ShapeDtypeStruct((pieces, pieces, rows // 2, 256), jnp.bfloat16)
    return pl.pallas_call(
        hidden_kernel,
        grid=(pieces,),
        in_specs=[
            pl.BlockSpec(tiles.shape, lambda i: (0, 0, 0)),
            pl.BlockSpec((rows, tokens.shape[1]), lambda i: (i, 0)),
        ],
        out_specs=[pl.BlockSpec(weight.shape, lambda i: (0, 0, 0))] * 2
        + [
            pl.BlockSpec((1, rows // 2, 224), lambda i: (i, 0, 0)),
            pl.BlockSpec((pieces, 1, rows // 2, 256), lambda i: (0, i, 0, 0)),
        ],
        out_shape=[weight, weight, even, odd],
        cost_estimate=pl.CostEstimate(
            flops=1900000000, bytes_accessed=8500000, transcendentals=230000
        ),
        compiler_params=pltpu.CompilerParams(
            dimension_semantics=("arbitrary",), vmem_limit_bytes=58 * 2**20
        ),
        name="hidden_units",
    )(tiles, tokens)


def out_kernel(*refs):
    out_ref = refs[-1]
    count = (len(refs) - 1) // 2
    for i in range(out_ref.shape[0]):
        total = jnp.dot(refs[0][i], refs[count][...], preferred_element_type=jnp.float32)
        for k in range(1, count):
            total = total + jnp.dot(
                refs[k][i], refs[count + k][...], preferred_element_type=jnp.float32
            )
        out_ref[i] = total.astype(out_ref.dtype)


def all_out_kernel(row_ref, hidden_ref, *refs):
    out_ref = refs[-1]
    count = hidden_ref.shape[0]
    for i in range(out_ref.shape[0]):
        total = jnp.dot(
            hidden_ref[row_ref[0], i, :, :224], refs[0][...], preferred_element_type=jnp.float32
        )
        for k in range(1, count):
            source = lax.rem(row_ref[0] + (count - k), count)
            total = total + jnp.dot(
                hidden_ref[source, i, :, :224], refs[k][...], preferred_element_type=jnp.float32
            )
        out_ref[i] = total.astype(out_ref.dtype)


def partial_out(hidden, down, kind, row=None):
    shape = (*hidden[0].shape[-3:-1], down[0].shape[1])
    whole = pl.BlockSpec(memory_space=pltpu.VMEM)
    first = [] if row is None else [row]
    return pl.pallas_call(
        out_kernel if row is None else all_out_kernel,
        in_specs=[pl.BlockSpec(memory_space=pltpu.SMEM)] * len(first)
        + [whole] * (len(hidden) + len(down)),
        out_specs=whole,
        out_shape=jax.ShapeDtypeStruct(shape, kind),
        cost_estimate=pl.CostEstimate(
            flops=470000000, bytes_accessed=3000000, transcendentals=0
        ),
        compiler_params=pltpu.CompilerParams(vmem_limit_bytes=12 * 2**20),
        name="partial_out",
    )(*first, *hidden, *down)


def permutation(sizes, move):
    groups, fs_0, fs_1, tp = sizes
    pairs = []
    for g in range(groups):
        for a in range(fs_0):
            for b in range(fs_1):
                for t in range(tp):
                    z, y = move(g * fs_0 + a, b, t)
                    z, y = z % (groups * fs_0), y % fs_1
                    pairs.append((((g * fs_0 + a) * fs_1 + b) * tp + t, (z * fs_1 + y) * tp + t))
    return pairs


def local(sizes, tokens, route_ids, route_logits, norm_gain, gate_master, up_master, down_master):
    f32, bf16 = jnp.float32, jnp.bfloat16
    fs_1, tp_size = sizes[2], sizes[3]

    def along_z(x, hops):
        pairs = permutation(sizes, lambda z, y, t: (z + (hops if t % 2 == 0 else -hops), y))
        return lax.ppermute(x, ALL, pairs)

    def along_y(x, hops):
        return lax.ppermute(x, ALL, permutation(sizes, lambda z, y, t: (z, y + hops)))

    as_float = tokens.astype(f32)
    normed = (
        as_float * lax.rsqrt(jnp.mean(as_float * as_float, axis=-1, keepdims=True) + EPS)
    ).astype(bf16)
    differ = route_logits[:, 0] - route_logits[:, 1]
    route_weight = jnp.stack([jax.nn.sigmoid(differ), jax.nn.sigmoid(-differ)], axis=1)
    expert_ids = jnp.arange(tp_size, dtype=jnp.int32)
    route_hits = route_ids[None, :, :] == expert_ids[:, None, None]
    chosen = jnp.any(route_hits, axis=2)
    slot_rank = jnp.cumsum(chosen.astype(jnp.int32), axis=1) - 1
    slot_ids = jnp.arange(CAP, dtype=jnp.int32)
    picker = chosen[:, None, :] & (slot_rank[:, None, :] == slot_ids[None, :, None])
    weight_rows = jnp.sum(jnp.where(route_hits, route_weight[None, :, :], 0.0), axis=2)
    mine = lax.axis_index("tp")
    my_picker = lax.dynamic_index_in_dim(picker, mine, 0, keepdims=False)
    slot_weight = jnp.sum(jnp.where(picker, weight_rows[:, None, :], 0.0), axis=2)
    packed = jnp.dot(my_picker.astype(bf16), normed, preferred_element_type=f32).astype(bf16)

    down_tiles = down_master.astype(bf16)
    down_tiles = lax.all_to_all(down_tiles, "tp", 0, 0, tiled=True)
    down_own = jnp.moveaxis(down_tiles, 0, 1).reshape(down_tiles.shape[1], -1)
    across = permutation(sizes, lambda z, y, t: (z + sizes[1], y))
    down_other = lax.ppermute(down_own, ALL, across)

    tiles = pack(gate_master, up_master, norm_gain[:, None])
    tiles = lax.all_to_all(tiles, "tp", 0, 0, tiled=True).reshape(-1, 112, LANES)
    tiles = jnp.concatenate([tiles, tiles], axis=0)
    tiles = lax.all_to_all(tiles, GR_FS, 0, 0, tiled=True)

    held = packed
    for hops in (4, 2, 1):
        moved = along_z(held, hops)
        held = jnp.concatenate([held, moved], axis=0)
    row = lax.axis_index("fs_1")
    gathered = jnp.zeros((fs_1, *held.shape), bf16)
    for k in range(fs_1):
        moved = held
        if k:
            moved = along_y(held, k)
        gathered = lax.dynamic_update_index_in_dim(gathered, moved, (row + fs_1 - k) % fs_1, 0)
    gathered = gathered.reshape(-1, gathered.shape[2])
    low = lax.axis_index("gr") == 0
    down_weight = jnp.concatenate(
        [jnp.where(low, down_own, down_other), jnp.where(low, down_other, down_own)], axis=1
    )
    columns = down_weight.shape[1] // fs_1
    down_cols = []
    for k in range(fs_1):
        picked = lax.dynamic_slice_in_dim(down_weight, (row + k) % fs_1 * columns, columns, axis=1)
        if k:
            picked = along_y(picked, k)
        down_cols.append(picked)
    tiles, gathered = lax.optimization_barrier((tiles, gathered))
    gate_weight, up_weight, even, odd = hidden_units(tiles, gathered, fs_1)

    odd = lax.all_to_all(odd, "fs_1", 0, 0, tiled=True)
    pieces = [even]
    for k in range(1, fs_1):
        pieces.append(along_y(even, k))
    odd = partial_out([odd], down_cols, bf16, row.astype(jnp.int32)[None])
    total = partial_out(pieces, down_cols, f32)
    for hops in (1, 2, 4):
        moved = along_z(odd.astype(bf16), -hops)
        total = total + moved.astype(f32)
        half = total.shape[1] // 2
        total, odd = total[:, :half], total[:, half:]
        if hops == 4:
            total = jnp.concatenate([total, odd], axis=1)

    block = total.astype(bf16)
    block = jnp.broadcast_to(block[:, None], (fs_1, tp_size, *block.shape[1:]))
    blocks = lax.all_to_all(block.reshape(-1, *block.shape[2:]), ("fs_1", "tp"), 0, 0, tiled=True)
    blocks = blocks.reshape(fs_1, -1, columns).astype(f32) * slot_weight.reshape(1, -1, 1)
    blocks = jnp.moveaxis(blocks.astype(bf16), 0, 1).reshape(-1, fs_1 * columns)
    mixed = lax.dot_general(
        picker.reshape(-1, picker.shape[2]).astype(bf16),
        blocks,
        (((0,), (0,)), ((), ())),
        preferred_element_type=f32,
    ).astype(bf16)
    return (gate_weight, up_weight, down_weight[None], mixed)


def solution(mesh):
    sizes = (mesh.shape["gr"], 8, 4, mesh.shape["tp"])
    torus = Mesh(mesh.devices.reshape(sizes), ALL)
    in_specs = (
        P(GR_FS, None),
        P(GR_FS, None),
        P(GR_FS, None),
        P(GR_FS),
        P(None, GR_FS, "tp"),
        P(None, GR_FS, "tp"),
        P(None, FS, ("gr", "tp")),
    )
    out_specs = (P("tp", None, FS), P("tp", None, FS), P("tp", FS, None), P(GR_FS, None))

    def call(*arrays):
        return local(sizes, *arrays)

    return jax.shard_map(call, mesh=torus, in_specs=in_specs, out_specs=out_specs, check_vma=False)
```

```python
import jax
import jax.numpy as jnp
from jax import lax
from jax.experimental import pallas as pl
from jax.experimental.pallas import tpu as pltpu
from jax.sharding import Mesh
from jax.sharding import PartitionSpec as P


CAP = 32
FS = ("fs_0", "fs_1")
GR_FS = ("gr", "fs_0", "fs_1")
ALL = ("gr", "fs_0", "fs_1", "tp")
EPS = 1e-06
LANES = 128


def lane_window(blocks, start):
    first, offset = divmod(start, LANES)
    if offset == 0:
        return blocks[first]
    head = pltpu.roll(blocks[first], LANES - offset, 1)
    if first + 1 == len(blocks):
        return head
    rest = pltpu.roll(blocks[first + 1], LANES - offset, 1)
    lane = lax.broadcasted_iota(jnp.int32, head.shape, 1)
    return jnp.where(lane < LANES - offset, head, rest)


def pack_kernel(gate_ref, up_ref, gain_ref, out_ref):
    gain = gain_ref[...]
    both = jnp.concatenate([gate_ref[0] * gain, up_ref[0] * gain], axis=0)
    blocks = [both[:, LANES * b : LANES * (b + 1)] for b in range(both.shape[1] // LANES)]
    lane = lax.broadcasted_iota(jnp.int32, (48, LANES), 1)
    for j in range(4):
        main = lane_window(blocks, 224 * j)
        tail = lane_window(blocks, 224 * j + LANES)
        last = tail[48:]
        spread = jnp.concatenate([pltpu.roll(last, 96 - 32 * q, 1) for q in range(3)], axis=0)
        out_ref[0, 112 * j : 112 * j + 64, :] = main.astype(jnp.bfloat16)
        out_ref[0, 112 * j + 64 : 112 * j + 112, :] = jnp.where(lane < 96, tail[:48], spread).astype(jnp.bfloat16)


def pack(gate_master, up_master, gain):
    experts, rows, cols = gate_master.shape
    return pl.pallas_call(
        pack_kernel,
        grid=(experts,),
        in_specs=[
            pl.BlockSpec((1, rows, cols), lambda i: (i, 0, 0)),
            pl.BlockSpec((1, rows, cols), lambda i: (i, 0, 0)),
            pl.BlockSpec((rows, 1), lambda i: (0, 0)),
        ],
        out_specs=pl.BlockSpec((1, 448, LANES), lambda i: (i, 0, 0)),
        out_shape=jax.ShapeDtypeStruct((experts, 448, LANES), jnp.bfloat16),
        cost_estimate=pl.CostEstimate(flops=4000000, bytes_accessed=2800000, transcendentals=0),
        compiler_params=pltpu.CompilerParams(vmem_limit_bytes=58 * 2**20),
        name="pack",
    )(gate_master, up_master, gain)


def hidden_kernel(tiles_ref, tokens_ref, gate_ref, up_ref, even_ref, odd_ref):
    @pl.when(pl.program_id(0) == 0)
    def _():
        lane = lax.broadcasted_iota(jnp.int32, (16, LANES), 1)

        for s in range(tiles_ref.shape[0]):
            rows = pl.ds(32 * s, 32)
            gate_ref[0, rows, :LANES] = tiles_ref[s, 0:32, :]
            up_ref[0, rows, :LANES] = tiles_ref[s, 32:64, :]
            gate_ref[0, rows, LANES:] = tiles_ref[s, 64:96, :96]
            up_ref[0, pl.ds(32 * s, 16), LANES:] = tiles_ref[s, 96:112, :96]
            parts = [
                pltpu.roll(
                    tiles_ref[s, 64 + 16 * q : 80 + 16 * q, :].astype(jnp.float32), 32 * q + 32, 1
                )
                for q in range(3)
            ]
            last = jnp.where(lane < 32, parts[0], jnp.where(lane < 64, parts[1], parts[2]))
            up_ref[0, pl.ds(32 * s + 16, 16), LANES:] = last[:, :96].astype(jnp.bfloat16)

    tokens = tokens_ref[...]
    gate = jnp.dot(tokens, gate_ref[0], preferred_element_type=jnp.float32)
    up = jnp.dot(tokens, up_ref[0], preferred_element_type=jnp.float32)
    hidden = (gate / (1.0 + jnp.exp(-gate)) * up).astype(jnp.bfloat16)
    half = hidden.shape[0] // 2
    even_ref[0] = hidden[:half]
    for k in range(odd_ref.shape[0]):
        odd_ref[k, 0, :, :224] = hidden[half:]
        odd_ref[k, 0, :, 224:] = jnp.zeros((half, 32), jnp.bfloat16)


def hidden_units(tiles, tokens, pieces):
    count = tiles.shape[0]
    rows = tokens.shape[0] // pieces
    weight = jax.ShapeDtypeStruct((1, 32 * count, 224), jnp.bfloat16)
    even = jax.ShapeDtypeStruct((pieces, rows // 2, 224), jnp.bfloat16)
    odd = jax.ShapeDtypeStruct((pieces, pieces, rows // 2, 256), jnp.bfloat16)
    return pl.pallas_call(
        hidden_kernel,
        grid=(pieces,),
        in_specs=[
            pl.BlockSpec(tiles.shape, lambda i: (0, 0, 0)),
            pl.BlockSpec((rows, tokens.shape[1]), lambda i: (i, 0)),
        ],
        out_specs=[pl.BlockSpec(weight.shape, lambda i: (0, 0, 0))] * 2
        + [
            pl.BlockSpec((1, rows // 2, 224), lambda i: (i, 0, 0)),
            pl.BlockSpec((pieces, 1, rows // 2, 256), lambda i: (0, i, 0, 0)),
        ],
        out_shape=[weight, weight, even, odd],
        cost_estimate=pl.CostEstimate(
            flops=1900000000, bytes_accessed=8500000, transcendentals=230000
        ),
        compiler_params=pltpu.CompilerParams(
            dimension_semantics=("arbitrary",), vmem_limit_bytes=58 * 2**20
        ),
        name="hidden_units",
    )(tiles, tokens)


def out_kernel(*refs):
    out_ref = refs[-1]
    count = (len(refs) - 1) // 2
    for i in range(out_ref.shape[0]):
        total = jnp.dot(refs[0][i], refs[count][...], preferred_element_type=jnp.float32)
        for k in range(1, count):
            total = total + jnp.dot(
                refs[k][i], refs[count + k][...], preferred_element_type=jnp.float32
            )
        out_ref[i] = total.astype(out_ref.dtype)


def all_out_kernel(row_ref, hidden_ref, *refs):
    out_ref = refs[-1]
    count = hidden_ref.shape[0]
    for i in range(out_ref.shape[0]):
        total = jnp.dot(
            hidden_ref[row_ref[0], i, :, :224], refs[0][...], preferred_element_type=jnp.float32
        )
        for k in range(1, count):
            source = lax.rem(row_ref[0] + (count - k), count)
            total = total + jnp.dot(
                hidden_ref[source, i, :, :224], refs[k][...], preferred_element_type=jnp.float32
            )
        out_ref[i] = total.astype(out_ref.dtype)


def partial_out(hidden, down, kind, row=None):
    shape = (*hidden[0].shape[-3:-1], down[0].shape[1])
    whole = pl.BlockSpec(memory_space=pltpu.VMEM)
    first = [] if row is None else [row]
    return pl.pallas_call(
        out_kernel if row is None else all_out_kernel,
        in_specs=[pl.BlockSpec(memory_space=pltpu.SMEM)] * len(first)
        + [whole] * (len(hidden) + len(down)),
        out_specs=whole,
        out_shape=jax.ShapeDtypeStruct(shape, kind),
        cost_estimate=pl.CostEstimate(
            flops=470000000, bytes_accessed=3000000, transcendentals=0
        ),
        compiler_params=pltpu.CompilerParams(vmem_limit_bytes=12 * 2**20),
        name="partial_out",
    )(*first, *hidden, *down)


def spread_kernel(total_ref, moved_ref, out_ref):
    block = (total_ref[...] + moved_ref[...].astype(jnp.float32)).astype(jnp.bfloat16)
    for t in range(out_ref.shape[1]):
        out_ref[:, t] = block


def spread(total, moved, copies):
    pieces, rows, columns = total.shape
    return pl.pallas_call(
        spread_kernel,
        out_shape=jax.ShapeDtypeStruct((pieces, copies, rows, columns), jnp.bfloat16),
        cost_estimate=pl.CostEstimate(flops=65536, bytes_accessed=1500000, transcendentals=0),
        compiler_params=pltpu.CompilerParams(vmem_limit_bytes=8 * 2**20),
        name="spread",
    )(total, moved)


def permutation(sizes, move):
    groups, fs_0, fs_1, tp = sizes
    pairs = []
    for g in range(groups):
        for a in range(fs_0):
            for b in range(fs_1):
                for t in range(tp):
                    z, y = move(g * fs_0 + a, b, t)
                    z, y = z % (groups * fs_0), y % fs_1
                    pairs.append((((g * fs_0 + a) * fs_1 + b) * tp + t, (z * fs_1 + y) * tp + t))
    return pairs


def local(sizes, tokens, route_ids, route_logits, norm_gain, gate_master, up_master, down_master):
    f32, bf16 = jnp.float32, jnp.bfloat16
    fs_1, tp_size = sizes[2], sizes[3]

    def along_z(x, hops):
        pairs = permutation(sizes, lambda z, y, t: (z + (hops if t % 2 == 0 else -hops), y))
        return lax.ppermute(x, ALL, pairs)

    def along_y(x, hops):
        return lax.ppermute(x, ALL, permutation(sizes, lambda z, y, t: (z, y + hops)))

    as_float = tokens.astype(f32)
    normed = (
        as_float * lax.rsqrt(jnp.mean(as_float * as_float, axis=-1, keepdims=True) + EPS)
    ).astype(bf16)
    differ = route_logits[:, 0] - route_logits[:, 1]
    route_weight = jnp.stack([jax.nn.sigmoid(differ), jax.nn.sigmoid(-differ)], axis=1)
    expert_ids = jnp.arange(tp_size, dtype=jnp.int32)
    route_hits = route_ids[None, :, :] == expert_ids[:, None, None]
    chosen = jnp.any(route_hits, axis=2)
    slot_rank = jnp.cumsum(chosen.astype(jnp.int32), axis=1) - 1
    slot_ids = jnp.arange(CAP, dtype=jnp.int32)
    picker = chosen[:, None, :] & (slot_rank[:, None, :] == slot_ids[None, :, None])
    weight_rows = jnp.sum(jnp.where(route_hits, route_weight[None, :, :], 0.0), axis=2)
    mine = lax.axis_index("tp")
    my_picker = lax.dynamic_index_in_dim(picker, mine, 0, keepdims=False)
    slot_weight = jnp.sum(jnp.where(picker, weight_rows[:, None, :], 0.0), axis=2)
    packed = jnp.dot(my_picker.astype(bf16), normed, preferred_element_type=f32).astype(bf16)

    down_tiles = down_master.astype(bf16)
    down_tiles = lax.all_to_all(down_tiles, "tp", 0, 0, tiled=True)
    down_own = jnp.moveaxis(down_tiles, 0, 1).reshape(down_tiles.shape[1], -1)
    across = permutation(sizes, lambda z, y, t: (z + sizes[1], y))
    down_other = lax.ppermute(down_own, ALL, across)

    tiles = pack(gate_master, up_master, norm_gain[:, None])
    tiles = lax.all_to_all(tiles, "tp", 0, 0, tiled=True).reshape(-1, 112, LANES)
    tiles = jnp.concatenate([tiles, tiles], axis=0)
    tiles = lax.all_to_all(tiles, GR_FS, 0, 0, tiled=True)

    held = packed
    for hops in (4, 2, 1):
        moved = along_z(held, hops)
        held = jnp.concatenate([held, moved], axis=0)
    row = lax.axis_index("fs_1")
    gathered = jnp.zeros((fs_1, *held.shape), bf16)
    for k in range(fs_1):
        moved = held
        if k:
            moved = along_y(held, k)
        gathered = lax.dynamic_update_index_in_dim(gathered, moved, (row + fs_1 - k) % fs_1, 0)
    gathered = gathered.reshape(-1, gathered.shape[2])
    low = lax.axis_index("gr") == 0
    down_weight = jnp.concatenate(
        [jnp.where(low, down_own, down_other), jnp.where(low, down_other, down_own)], axis=1
    )
    columns = down_weight.shape[1] // fs_1
    down_cols = []
    for k in range(fs_1):
        picked = lax.dynamic_slice_in_dim(down_weight, (row + k) % fs_1 * columns, columns, axis=1)
        if k:
            picked = along_y(picked, k)
        down_cols.append(picked)
    tiles, gathered = lax.optimization_barrier((tiles, gathered))
    gate_weight, up_weight, even, odd = hidden_units(tiles, gathered, fs_1)

    odd = lax.all_to_all(odd, "fs_1", 0, 0, tiled=True)
    pieces = [even]
    for k in range(1, fs_1):
        pieces.append(along_y(even, k))
    odd = partial_out([odd], down_cols, bf16, row.astype(jnp.int32)[None])
    total = partial_out(pieces, down_cols, f32)
    for hops in (1, 2, 4):
        moved = along_z(odd.astype(bf16), -hops)
        if hops == 4:
            block = spread(total, moved, tp_size)
        else:
            total = total + moved.astype(f32)
            half = total.shape[1] // 2
            total, odd = total[:, :half], total[:, half:]

    blocks = lax.all_to_all(block.reshape(-1, *block.shape[2:]), ("fs_1", "tp"), 0, 0, tiled=True)
    blocks = blocks.reshape(fs_1, -1, columns).astype(f32) * slot_weight.reshape(1, -1, 1)
    blocks = jnp.moveaxis(blocks.astype(bf16), 0, 1).reshape(-1, fs_1 * columns)
    mixed = lax.dot_general(
        picker.reshape(-1, picker.shape[2]).astype(bf16),
        blocks,
        (((0,), (0,)), ((), ())),
        preferred_element_type=f32,
    ).astype(bf16)
    return (gate_weight, up_weight, down_weight[None], mixed)


def solution(mesh):
    sizes = (mesh.shape["gr"], 8, 4, mesh.shape["tp"])
    torus = Mesh(mesh.devices.reshape(sizes), ALL)
    in_specs = (
        P(GR_FS, None),
        P(GR_FS, None),
        P(GR_FS, None),
        P(GR_FS),
        P(None, GR_FS, "tp"),
        P(None, GR_FS, "tp"),
        P(None, FS, ("gr", "tp")),
    )
    out_specs = (P("tp", None, FS), P("tp", None, FS), P("tp", FS, None), P(GR_FS, None))

    def call(*arrays):
        return local(sizes, *arrays)

    return jax.shard_map(call, mesh=torus, in_specs=in_specs, out_specs=out_specs, check_vma=False)
```
